32 devices in a mesh: sp: 4 (over z), fs: 4 (over y, x), tp: 2 (over core).
Axes of the slice: x: 2, y: 2, z: 4, core: 2. Of those that a mesh axis runs over, the one named last changes fastest.
Arguments:
- stream: bfloat16 [4, 1024, 4096], P('fs', 'sp'), may hold values from -6 to 6
- norm_gain: float32 [4096], replicated, may hold values from 0.1 to 1.9
- value_proj: bfloat16 [4096, 1024], P(('sp', 'fs'), 'tp'), may hold values from -0.09375 to 0.09375
- gate_proj: bfloat16 [4096, 1024], P(('sp', 'fs'), 'tp'), may hold values from -0.09375 to 0.09375
- state_proj: bfloat16 [4096, 1024], P(('sp', 'fs'), 'tp'), may hold values from -0.09375 to 0.09375
- conv_kernel: bfloat16 [31, 1024], P(None, 'tp'), may hold values from -1 to 1
- conv_gain: float32 [1024], P('tp'), may hold values from 0.1 to 1.9
- decay_rate: float32 [64, 64], P('tp'), may hold values from 0.25 to 1
- frequency: float32 [64, 64], P('tp'), may hold values from 0 to 201.06177
- log_step: float32 [64], P('tp'), may hold values from -12 to -2.3
- step_gain: float32 [4, 64, 1024], P('fs', 'tp', 'sp'), may hold values from 0.35 to 614.4
- drive_matrix: float32 [2, 64, 64, 16], P(None, 'tp'), may hold values from -1 to 1
- read_matrix: float32 [2, 64, 16, 64], P(None, 'tp'), may hold values from -0.5 to 0.5
- skip_gain: float32 [1024], P('tp'), may hold values from -4 to 4
- start_state: float32 [2, 4, 64, 64], P(None, 'fs', 'tp'), may hold values from -6 to 6
- merge_conv: bfloat16 [4096, 1024], P(('sp', 'fs'), 'tp'), may hold values from -0.125 to 0.125
- merge_state: bfloat16 [4096, 1024], P(('sp', 'fs'), 'tp'), may hold values from -0.125 to 0.125
Outputs:
- mixed: bfloat16 [4, 1024, 4096], P('fs', ('sp', 'tp'))
The draws below stay inside these ranges and needn't reach their ends.
All inputs are finite; a program needn't handle non-finite values.
Results may differ from the reference program's by a relative error of at most 0.014.
Values may be sent and summed in bfloat16 or wider, within the bound.
A program may use at most 256 MiB of HBM per device.

```python
import math
import jax
import jax.numpy as jnp
from jax import lax

D = 4096
CONV_HEADS = 8
HEAD_CH = 128
GROUPS = 64
GROUP_CH = 16
STATE = 64
KERNEL = 31
TOK_DEV = 256
SEQUENCE_COUNT = 4
SEQUENCE_LENGTH = 1024
CONV_CH = 1024
SCAN_CH = 1024
HEAD_BLOCKS = 2


def draw_log_step(key, part):
    ranking = jax.random.permutation(jax.random.fold_in(key, 11), GROUPS)
    slow_count = GROUPS // 2
    slow_mask = ranking < slow_count
    slow_value = jnp.log(jax.random.uniform(jax.random.fold_in(key, 12), (GROUPS,), jnp.float32, 0.2, 0.8) / SEQUENCE_LENGTH)
    fast_value = jnp.log(jax.random.uniform(jax.random.fold_in(key, 13), (GROUPS,), jnp.float32, 0.05, 0.1))
    return jnp.where(slow_mask, slow_value, fast_value).astype(jnp.float32)


def draw_step_gain(key, part):
    block_count = SEQUENCE_LENGTH // TOK_DEV
    per_block = jnp.exp(jax.random.uniform(jax.random.fold_in(key, 21), (SEQUENCE_COUNT, GROUPS, block_count), jnp.float32, math.log(0.5), math.log(2.0)))
    smooth_signal = jnp.repeat(per_block, TOK_DEV, axis=2)
    noisy_signal = jnp.exp(jax.random.uniform(jax.random.fold_in(key, 22), (SEQUENCE_COUNT, GROUPS, SEQUENCE_LENGTH), jnp.float32, math.log(0.7), math.log(1.4)))
    spike_positions = jax.random.randint(jax.random.fold_in(key, 23), (SEQUENCE_COUNT, 3), 0, SEQUENCE_LENGTH)
    position_index = jnp.arange(SEQUENCE_LENGTH, dtype=jnp.int32)
    spike_mask = jnp.any(position_index[None, None, :] == spike_positions[:, :, None], axis=1)
    spike_values = SEQUENCE_LENGTH * jax.random.uniform(jax.random.fold_in(key, 24), (SEQUENCE_COUNT, 1, SEQUENCE_LENGTH), jnp.float32, 0.25, 0.6)
    return jnp.where(spike_mask[:, None, :], spike_values, smooth_signal * noisy_signal).astype(jnp.float32)


def block_scale(rng, dims, pieces, low, top_value):
    def one(dim, shards_of):
        steps = jax.random.uniform(jax.random.fold_in(jax.random.fold_in(rng, 6), dim), (shards_of,), jnp.float32, low / len(pieces), top_value / len(pieces))
        return jnp.repeat(jnp.exp(steps), dims[dim] // shards_of).reshape((-1,) + (1,) * (len(dims) - dim - 1))

    loudness = one(*pieces[0])
    for cut in pieces[1:]:
        loudness = loudness * one(*cut)
    return loudness


def bell_draw(key, extent, deviation, most, split=(), held_as=jnp.bfloat16):
    gain = block_scale(key, extent, split, -0.22, 0.18) if split else 1.0
    result = jax.random.normal(key, extent, jnp.float32) * deviation * gain
    return jnp.minimum(jnp.maximum(result, -most), most).astype(held_as)


def setup_inputs(seed: int = 0) -> dict:
    key_list = jax.random.split(jax.random.key(seed), 18)
    return {
        "stream": bell_draw(key_list[0], (SEQUENCE_COUNT, SEQUENCE_LENGTH, D), 1.0, 6.0, ((0, 4), (1, 4))),
        "norm_gain": jnp.clip(1.0 + 0.18 * jax.random.normal(key_list[1], (D,), jnp.float32), 0.1, 1.9),
        "value_proj": bell_draw(key_list[2], (D, CONV_CH), D ** -0.5, 0.09375, ((0, 16), (1, 2))),
        "gate_proj": bell_draw(key_list[3], (D, CONV_CH), D ** -0.5, 0.09375, ((0, 16), (1, 2))),
        "state_proj": bell_draw(key_list[4], (D, SCAN_CH), D ** -0.5, 0.09375, ((0, 16), (1, 2))),
        "conv_kernel": bell_draw(key_list[5], (KERNEL, CONV_CH), KERNEL ** -0.5, 1.0, ((1, 2),)),
        "conv_gain": jnp.clip(1.0 + 0.18 * jax.random.normal(key_list[6], (CONV_CH,), jnp.float32), 0.1, 1.9),
        "decay_rate": jnp.clip(jnp.exp(math.log(1.0) - 1.3862944 * jax.random.uniform(key_list[7], (GROUPS, STATE), jnp.float32) ** block_scale(key_list[7], (GROUPS, STATE), ((0, 2),), -0.2, 0.2)), 0.25, 1.0),
        "frequency": jnp.clip(201.06177 * jax.random.uniform(key_list[8], (GROUPS, STATE), jnp.float32) ** block_scale(key_list[8], (GROUPS, STATE), ((0, 2),), -0.2, 0.2), 0.0, 201.06177),
        "log_step": draw_log_step(jax.random.fold_in(key_list[17], 71), 0),
        "step_gain": draw_step_gain(jax.random.fold_in(key_list[17], 71), 0),
        "drive_matrix": bell_draw(key_list[11], (2, GROUPS, STATE, GROUP_CH), (2 * GROUP_CH) ** -0.5, 1.0, ((1, 2),), jnp.float32),
        "read_matrix": bell_draw(key_list[12], (2, GROUPS, GROUP_CH, STATE), (2 * STATE) ** -0.5, 0.5, ((1, 2),), jnp.float32),
        "skip_gain": bell_draw(key_list[13], (SCAN_CH,), 1.0, 4.0, ((0, 2),), jnp.float32),
        "start_state": bell_draw(key_list[14], (2, SEQUENCE_COUNT, GROUPS, STATE), 1.0, 6.0, ((1, 4), (2, 2)), jnp.float32),
        "merge_conv": bell_draw(key_list[15], (D, CONV_CH), (CONV_CH + SCAN_CH) ** -0.5, 0.125, ((0, 16), (1, 2))),
        "merge_state": bell_draw(key_list[16], (D, SCAN_CH), (CONV_CH + SCAN_CH) ** -0.5, 0.125, ((0, 16), (1, 2))),
    }


exact_mode = lax.Precision.HIGHEST

def reference(stream, norm_gain, value_proj, gate_proj, state_proj, conv_kernel, conv_gain, decay_rate, frequency, log_step, step_gain, drive_matrix, read_matrix, skip_gain, start_state, merge_conv, merge_state):
    widened = stream.astype(jnp.float32)
    inverse = lax.rsqrt(lax.optimization_barrier(jnp.mean(widened * widened, axis=2, keepdims=True)) + 1e-06)
    normed = (widened * inverse * norm_gain).astype(jnp.bfloat16).reshape(SEQUENCE_COUNT * SEQUENCE_LENGTH, D)
    value_pre = jnp.dot(normed, value_proj, preferred_element_type=jnp.float32)
    gate_pre = jnp.dot(normed, gate_proj, preferred_element_type=jnp.float32)
    gated = (value_pre * jax.nn.sigmoid(gate_pre)).astype(jnp.bfloat16).reshape(SEQUENCE_COUNT, SEQUENCE_LENGTH, CONV_CH)
    scan_input = jnp.dot(normed, state_proj, preferred_element_type=jnp.float32).astype(jnp.bfloat16)
    scan_input = scan_input.reshape(SEQUENCE_COUNT, SEQUENCE_LENGTH, SCAN_CH)
    margin = KERNEL - 1
    padded = jnp.pad(gated, ((0, 0), (margin, 0), (0, 0))).astype(jnp.float32)
    kernel = conv_kernel.astype(jnp.float32)
    mixed_taps = jnp.zeros((SEQUENCE_COUNT, SEQUENCE_LENGTH, CONV_CH), jnp.float32)
    for tap_index in range(KERNEL):
        mixed_taps = mixed_taps + kernel[tap_index] * padded[:, tap_index:tap_index + SEQUENCE_LENGTH]
    grouped = mixed_taps.reshape(SEQUENCE_COUNT, SEQUENCE_LENGTH, CONV_HEADS, HEAD_CH)
    center = grouped - lax.optimization_barrier(jnp.mean(grouped, axis=3, keepdims=True))
    spread = lax.optimization_barrier(jnp.mean(center * center, axis=3, keepdims=True))
    normal = (center * lax.rsqrt(spread + 1e-05)).reshape(SEQUENCE_COUNT, SEQUENCE_LENGTH, CONV_CH) * conv_gain
    conv_out = (normal * jax.nn.sigmoid(normal)).astype(jnp.bfloat16)
    base_step = jnp.exp(log_step)
    magnitude = decay_rate * decay_rate + frequency * frequency

    def advance(carry, inputs):
        state_re, state_im = carry
        gain_now, input_now = inputs
        step_size = (base_step * gain_now)[:, :, None]
        modulus = jnp.exp(-step_size * decay_rate)
        rotation = step_size * frequency
        trans_re = modulus * jnp.cos(rotation)
        trans_im = modulus * jnp.sin(rotation)
        less_re = trans_re - 1.0
        factor_re = (-decay_rate * less_re + frequency * trans_im) / magnitude
        factor_im = (-decay_rate * trans_im - frequency * less_re) / magnitude
        grouped_in = input_now.astype(jnp.float32).reshape(SEQUENCE_COUNT, GROUPS, GROUP_CH)
        drive_re = jnp.einsum('gnc,sgc->sgn', drive_matrix[0], grouped_in, precision=exact_mode)
        drive_im = jnp.einsum('gnc,sgc->sgn', drive_matrix[1], grouped_in, precision=exact_mode)
        push_re = factor_re * drive_re - factor_im * drive_im
        push_im = factor_re * drive_im + factor_im * drive_re
        new_re = trans_re * state_re - trans_im * state_im + push_re
        new_im = trans_re * state_im + trans_im * state_re + push_im
        read_out = jnp.einsum('gcn,sgn->sgc', read_matrix[0], new_re, precision=exact_mode) - jnp.einsum('gcn,sgn->sgc', read_matrix[1], new_im, precision=exact_mode)
        return ((new_re, new_im), read_out)
    gains_by_pos = jnp.transpose(step_gain, (2, 0, 1))
    inputs_by_pos = jnp.transpose(scan_input, (1, 0, 2))
    unused, read_all = lax.scan(advance, (start_state[0], start_state[1]), (gains_by_pos, inputs_by_pos))
    read_all = jnp.transpose(read_all, (1, 0, 2, 3)).reshape(SEQUENCE_COUNT, SEQUENCE_LENGTH, SCAN_CH)
    state_out = jax.nn.gelu(read_all + skip_gain * scan_input.astype(jnp.float32)).astype(jnp.bfloat16)
    conv_rows = conv_out.reshape(SEQUENCE_COUNT * SEQUENCE_LENGTH, CONV_CH)
    state_rows = state_out.reshape(SEQUENCE_COUNT * SEQUENCE_LENGTH, SCAN_CH)
    conv_block = CONV_CH // HEAD_BLOCKS
    scan_block = SCAN_CH // HEAD_BLOCKS
    contract = (((1,), (1,)), ((), ()))
    total = jnp.zeros((SEQUENCE_COUNT * SEQUENCE_LENGTH, D), jnp.float32)
    for block_index in range(HEAD_BLOCKS):
        conv_lo = block_index * conv_block
        scan_lo = block_index * scan_block
        block_sum = lax.dot_general(conv_rows[:, conv_lo:conv_lo + conv_block], merge_conv[:, conv_lo:conv_lo + conv_block], contract, preferred_element_type=jnp.float32)
        block_sum = block_sum + lax.dot_general(state_rows[:, scan_lo:scan_lo + scan_block], merge_state[:, scan_lo:scan_lo + scan_block], contract, preferred_element_type=jnp.float32)
        rounded = lax.optimization_barrier(block_sum.astype(jnp.bfloat16))
        total = total + rounded.astype(jnp.float32)
    return total.astype(jnp.bfloat16).reshape(SEQUENCE_COUNT, SEQUENCE_LENGTH, D)
```

```python
import functools

import jax
import jax.numpy as jnp
from jax import lax
from jax.experimental import pallas as pl
from jax.experimental.pallas import tpu as pltpu
from jax.sharding import PartitionSpec as P

HEAD_CH = 128
LANES = 128
CHUNKS = 8


def shifted(value, axis, steps):
    count = lax.axis_size(axis)
    initial, last = (max(0, -steps), min(count, count - steps))
    return lax.ppermute(value, axis, [(source, source + steps) for source in range(initial, last)])


def order_matrix(rows, transposed):
    length = rows // CHUNKS
    first = lax.broadcasted_iota(jnp.int32, (rows, rows), 0)
    second = lax.broadcasted_iota(jnp.int32, (rows, rows), 1)
    mixed, position = (second, first) if transposed else (first, second)
    hit = position == (mixed % CHUNKS) * length + mixed // CHUNKS
    return hit.astype(jnp.float32).astype(jnp.bfloat16)


def turn(angle):
    count = (angle * 0.6366197723675814 + 0.5).astype(jnp.int32)
    whole = count.astype(jnp.float32)
    rest = angle - whole * 1.5703125
    rest = rest - whole * 4.837512969970703125e-4
    rest = rest - whole * 7.54978995489188216e-8
    square = rest * rest
    sine = rest + rest * square * (
        -1.6666654611e-1 + square * (8.3321608736e-3 + square * -1.9515295891e-4)
    )
    less = square * (
        -0.5
        + square
        * (4.166664568298827e-2 + square * (-1.388731625493765e-3 + square * 2.443315711809948e-5))
    )
    cosine = 1.0 + less
    odd = (count & 1) == 1
    sin_out = jnp.where(odd, cosine, sine)
    cos_out = jnp.where(odd, sine, cosine)
    sin_out = jnp.where((count & 2) == 2, -sin_out, sin_out)
    cos_out = jnp.where(((count + 1) & 2) == 2, -cos_out, cos_out)
    less_out = jnp.where((count & 3) == 0, less, cos_out - 1.0)
    return less_out, cos_out, sin_out


def scan_kernel(
    x_ref, step_ref, spread_ref, lam_ref, high_ref, low_ref,
    are_ref, aim_ref, sre_ref, sim_ref, chunk_ref, total_ref,
    wide_ref, drive_ref,
):
    rows = x_ref.shape[0]
    width = lam_ref.shape[2]
    order = order_matrix(rows, False)
    x = jnp.dot(order, x_ref[...], preferred_element_type=jnp.float32).astype(jnp.bfloat16)
    drive_ref[...] = jnp.dot(x, high_ref[0], preferred_element_type=jnp.float32) + jnp.dot(
        x, low_ref[0], preferred_element_type=jnp.float32
    )
    wide_ref[...] = jnp.dot(
        step_ref[0], spread_ref[...], precision=lax.Precision.HIGHEST,
        preferred_element_type=jnp.float32,
    )

    def one(i, carry):
        here = pl.ds(pl.multiple_of(i * CHUNKS, CHUNKS), CHUNKS)
        results = []
        for j in range(width // LANES):
            a_re, a_im, s_re, s_im = carry[j]
            cols = slice(j * LANES, (j + 1) * LANES)
            step = wide_ref[here, cols]
            rate = lam_ref[0, 0:1, cols]
            freq = lam_ref[0, 1:2, cols]
            inv_re = lam_ref[0, 2:3, cols]
            inv_im = lam_ref[0, 3:4, cols]
            decay = -step * rate
            series = decay * (
                1.0 + decay * (0.5 + decay * (
                    1.0 / 6 + decay * (1.0 / 24 + decay * (1.0 / 120 + decay * (1.0 / 720)))
                ))
            )
            fall = jnp.where(decay > -0.25, series, jnp.exp(decay) - 1.0)
            modulus = 1.0 + fall
            modulus = jnp.where(decay > -0.25, modulus, jnp.exp(decay))
            cos_less, cosine, sine = turn(step * freq)
            t_re = modulus * cosine
            t_im = modulus * sine
            less = fall * cosine + cos_less
            f_re = less * inv_re - t_im * inv_im
            f_im = less * inv_im + t_im * inv_re
            d_re = drive_ref[here, cols]
            d_im = drive_ref[here, slice(width + j * LANES, width + (j + 1) * LANES)]
            p_re = f_re * d_re - f_im * d_im
            p_im = f_re * d_im + f_im * d_re
            s_re, s_im = t_re * s_re - t_im * s_im + p_re, t_re * s_im + t_im * s_re + p_im
            a_re, a_im = t_re * a_re - t_im * a_im, t_re * a_im + t_im * a_re
            are_ref[0, here, cols] = a_re
            aim_ref[0, here, cols] = a_im
            sre_ref[0, here, cols] = s_re
            sim_ref[0, here, cols] = s_im
            results.append((a_re, a_im, s_re, s_im))
        return tuple(results)

    ones = jnp.ones((CHUNKS, LANES), jnp.float32)
    zeros = jnp.zeros((CHUNKS, LANES), jnp.float32)
    start = tuple((ones, zeros, zeros, zeros) for _ in range(width // LANES))
    ends = lax.fori_loop(0, rows // CHUNKS, one, start)
    place = lax.broadcasted_iota(jnp.int32, (CHUNKS, LANES), 0)
    for j in range(width // LANES):
        cols = slice(j * LANES, (j + 1) * LANES)
        current = (ones[0:1], zeros[0:1], zeros[0:1], zeros[0:1])
        kept = [zeros] * 4
        for c in range(CHUNKS):
            kept = [jnp.where(place == c, v, k) for v, k in zip(current, kept)]
            t_re, t_im, p_re, p_im = (e[c : c + 1] for e in ends[j])
            a_re, a_im, s_re, s_im = current
            current = (
                t_re * a_re - t_im * a_im,
                t_re * a_im + t_im * a_re,
                t_re * s_re - t_im * s_im + p_re,
                t_re * s_im + t_im * s_re + p_im,
            )
        for q in range(4):
            chunk_ref[0, q, :, cols] = kept[q]
            total_ref[0, q : q + 1, cols] = current[q]


def read_kernel(
    are_ref, aim_ref, sre_ref, sim_ref, chunk_ref, enter_ref, x_ref, skip_ref, high_ref, low_ref,
    out_ref, state_ref,
):
    rows = x_ref.shape[0]
    width = are_ref.shape[2]
    e_re = enter_ref[0, 0:1, :]
    e_im = enter_ref[0, 1:2, :]
    a_re, a_im = chunk_ref[0, 0], chunk_ref[0, 1]
    c_re = a_re * e_re - a_im * e_im + chunk_ref[0, 2]
    c_im = a_re * e_im + a_im * e_re + chunk_ref[0, 3]

    def one(i, carry):
        here = pl.ds(pl.multiple_of(i * CHUNKS, CHUNKS), CHUNKS)
        a_re = are_ref[0, here, :]
        a_im = aim_ref[0, here, :]
        state_ref[here, 0:width] = sre_ref[0, here, :] + a_re * c_re - a_im * c_im
        state_ref[here, width : 2 * width] = sim_ref[0, here, :] + a_re * c_im + a_im * c_re
        return carry

    lax.fori_loop(0, rows // CHUNKS, one, 0)
    state = state_ref[...]
    high = state.astype(jnp.bfloat16)
    low = (state - high.astype(jnp.float32)).astype(jnp.bfloat16)
    read = (
        jnp.dot(high, high_ref[0], preferred_element_type=jnp.float32)
        + jnp.dot(low, high_ref[0], preferred_element_type=jnp.float32)
        + jnp.dot(high, low_ref[0], preferred_element_type=jnp.float32)
    )
    x = jnp.dot(order_matrix(rows, False), x_ref[...], preferred_element_type=jnp.float32)
    out = jax.nn.gelu(read + skip_ref[...] * x).astype(jnp.bfloat16)
    out_ref[...] = jnp.dot(
        order_matrix(rows, True), out, preferred_element_type=jnp.float32
    ).astype(jnp.bfloat16)


def conv_kernel_body(gated_ref, before_ref, taps_ref, gain_ref, out_ref, pad_ref):
    rows = gated_ref.shape[0]
    lead = before_ref.shape[0]
    count = taps_ref.shape[0]
    pad_ref[0:lead, :] = before_ref[...].astype(jnp.float32)
    pad_ref[lead:, :] = gated_ref[...].astype(jnp.float32)
    slab = 64
    for r in range(0, rows, slab):
        total = jnp.zeros((slab, LANES), jnp.float32)
        for k in range(count):
            begin = r + lead - (count - 1) + k
            total = total + taps_ref[k : k + 1, :] * pad_ref[begin : begin + slab, :]
        center = total - jnp.mean(total, axis=1, keepdims=True)
        spread = jnp.mean(center * center, axis=1, keepdims=True)
        value = center * lax.rsqrt(spread + 1e-05) * gain_ref[...]
        out_ref[r : r + slab, :] = (value * jax.nn.sigmoid(value)).astype(jnp.bfloat16)


def split(value):
    high = value.astype(jnp.bfloat16)
    low = (value - high.astype(jnp.float32)).astype(jnp.bfloat16)
    return high, low


def cost(flops, size):
    return pl.CostEstimate(flops=flops, bytes_accessed=size, transcendentals=0)


def body(
    stream, norm_gain, value_proj, gate_proj, state_proj, conv_kernel, conv_gain, decay_rate,
    frequency, log_step, step_gain, drive_matrix, read_matrix, skip_gain, start_state,
    merge_conv, merge_state,
):
    rows = stream.shape[1]
    groups, states = decay_rate.shape
    per = drive_matrix.shape[3]
    pack = min(groups, LANES // per)
    blocks = groups // pack
    width = pack * states
    chans = pack * per
    f32 = jnp.float32

    state_whole = lax.all_gather(state_proj, ("sp", "fs"), axis=0, tiled=True)
    value_whole = lax.all_gather(value_proj, ("sp", "fs"), axis=0, tiled=True)
    gate_whole = lax.all_gather(gate_proj, ("sp", "fs"), axis=0, tiled=True)
    conv_merge = lax.all_gather(merge_conv, ("sp", "fs"), axis=0, tiled=True)
    state_merge = lax.all_gather(merge_state, ("sp", "fs"), axis=0, tiled=True)

    widened = stream[0].astype(f32)
    inverse = lax.rsqrt(jnp.mean(widened * widened, axis=1, keepdims=True) + 1e-06)
    normed = (widened * inverse * norm_gain).astype(jnp.bfloat16)

    step = (jnp.exp(log_step)[:, None] * step_gain[0]).reshape(
        blocks, pack, CHUNKS, rows // CHUNKS
    )
    step = jnp.transpose(step, (0, 3, 2, 1)).reshape(blocks, rows, pack)
    spread = jnp.repeat(jnp.eye(pack, dtype=f32), states, axis=1)
    magnitude = decay_rate * decay_rate + frequency * frequency
    lam = jnp.stack(
        [decay_rate, frequency, -decay_rate / magnitude, -frequency / magnitude]
    ).reshape(4, blocks, width)
    lam = jnp.transpose(lam, (1, 0, 2))
    same = jnp.eye(pack, dtype=f32)
    drive = jnp.transpose(drive_matrix.reshape(2, blocks, pack, states, per), (1, 2, 4, 0, 3))
    drive = drive[:, :, :, :, None, :] * same[None, :, None, None, :, None]
    drive_high, drive_low = split(drive.reshape(blocks, chans, 2 * width))
    signed = jnp.stack([read_matrix[0], -read_matrix[1]])
    read = jnp.transpose(signed.reshape(2, blocks, pack, per, states), (1, 0, 2, 4, 3))
    read = read[:, :, :, :, None, :] * same[None, None, :, None, :, None]
    read_high, read_low = split(read.reshape(blocks, 2 * width, chans))

    scan_input = jnp.dot(normed, state_whole, preferred_element_type=f32).astype(jnp.bfloat16)

    def slab(*shape):
        return pl.BlockSpec((1,) + shape, lambda b: (b,) + (0,) * len(shape))

    chan_spec = pl.BlockSpec((rows, chans), lambda b: (0, b))
    row_spec = pl.BlockSpec((1, chans), lambda b: (0, b))
    wide = jax.ShapeDtypeStruct((blocks, rows, width), f32)
    *running, chunk, total = pl.pallas_call(
        scan_kernel,
        grid=(blocks,),
        in_specs=[
            chan_spec, slab(rows, pack), pl.BlockSpec((pack, width), lambda b: (0, 0)),
            slab(4, width), slab(chans, 2 * width), slab(chans, 2 * width),
        ],
        out_specs=[slab(rows, width)] * 4 + [slab(4, CHUNKS, width), slab(4, width)],
        out_shape=[wide] * 4 + [
            jax.ShapeDtypeStruct((blocks, 4, CHUNKS, width), f32),
            jax.ShapeDtypeStruct((blocks, 4, width), f32),
        ],
        scratch_shapes=[pltpu.VMEM((rows, width), f32), pltpu.VMEM((rows, 2 * width), f32)],
        cost_estimate=cost(60 * rows * blocks * width * 30, 16 * rows * blocks * width),
        name="scan",
    )(scan_input, step, spread, lam, drive_high, drive_low)

    place = lax.axis_index("sp")
    arrived = [
        (hop, shifted(total, "sp", hop)) for hop in range(lax.axis_size("sp") - 1, 0, -1)
    ]
    begin = start_state[:, 0].reshape(2, blocks, width)
    enter_re, enter_im = begin[0], begin[1]
    for hop, part in arrived:
        t_re, t_im, p_re, p_im = (part[:, q] for q in range(4))
        known = place >= hop
        next_re = t_re * enter_re - t_im * enter_im + p_re
        next_im = t_re * enter_im + t_im * enter_re + p_im
        enter_re = jnp.where(known, next_re, enter_re)
        enter_im = jnp.where(known, next_im, enter_im)
    enter = jnp.stack([enter_re, enter_im], axis=1)

    state_out = pl.pallas_call(
        read_kernel,
        grid=(blocks,),
        in_specs=[slab(rows, width)] * 4 + [
            slab(4, CHUNKS, width), slab(2, width), chan_spec, row_spec,
            slab(2 * width, chans), slab(2 * width, chans),
        ],
        out_specs=chan_spec,
        out_shape=jax.ShapeDtypeStruct((rows, groups * per), jnp.bfloat16),
        scratch_shapes=[pltpu.VMEM((rows, 2 * width), f32)],
        cost_estimate=cost(60 * rows * blocks * width * 10, 16 * rows * blocks * width),
        name="read",
    )(*running, chunk, enter, scan_input, skip_gain[None], read_high, read_low)

    value_pre = jnp.dot(normed, value_whole, preferred_element_type=f32)
    gate_pre = jnp.dot(normed, gate_whole, preferred_element_type=f32)
    gated = (value_pre * jax.nn.sigmoid(gate_pre)).astype(jnp.bfloat16)
    lead = -(-(conv_kernel.shape[0] - 1) // 16) * 16
    before = shifted(gated[rows - lead :], "sp", 1)
    conv_width = gated.shape[1]
    head_spec = lambda n: pl.BlockSpec((n, HEAD_CH), lambda h: (0, h))
    conv_out = pl.pallas_call(
        conv_kernel_body,
        grid=(conv_width // HEAD_CH,),
        in_specs=[
            head_spec(rows), head_spec(lead), head_spec(conv_kernel.shape[0]), head_spec(1),
        ],
        out_specs=head_spec(rows),
        out_shape=jax.ShapeDtypeStruct((rows, conv_width), jnp.bfloat16),
        scratch_shapes=[pltpu.VMEM((rows + lead, HEAD_CH), f32)],
        cost_estimate=cost(rows * conv_width * 2000, 4 * rows * conv_width),
        name="conv",
    )(gated, before, conv_kernel.astype(f32), conv_gain[None])

    contract = (((1,), (1,)), ((), ()))
    conv_term = lax.dot_general(conv_out, conv_merge, contract, preferred_element_type=f32)
    state_term = lax.dot_general(state_out, state_merge, contract, preferred_element_type=f32)
    mixed = lax.psum_scatter(
        (conv_term + state_term).astype(jnp.bfloat16), "tp", scatter_dimension=0, tiled=True
    )
    return mixed[None]


def solution(mesh):
    return jax.shard_map(
        body,
        mesh=mesh,
        in_specs=(
            P("fs", "sp", None),
            P(),
            P(("sp", "fs"), "tp"),
            P(("sp", "fs"), "tp"),
            P(("sp", "fs"), "tp"),
            P(None, "tp"),
            P("tp"),
            P("tp", None),
            P("tp", None),
            P("tp"),
            P("fs", "tp", "sp"),
            P(None, "tp", None, None),
            P(None, "tp", None, None),
            P("tp"),
            P(None, "fs", "tp", None),
            P(("sp", "fs"), "tp"),
            P(("sp", "fs"), "tp"),
        ),
        out_specs=P("fs", ("sp", "tp"), None),
        check_vma=False,
    )
```

```python
import functools

import jax
import jax.numpy as jnp
from jax import lax
from jax.experimental import pallas as pl
from jax.experimental.pallas import tpu as pltpu
from jax.sharding import PartitionSpec as P

HEAD_CH = 128
LANES = 128
CHUNKS = 8


def shifted(value, axis, steps):
    count = lax.axis_size(axis)
    initial, last = (max(0, -steps), min(count, count - steps))
    return lax.ppermute(value, axis, [(source, source + steps) for source in range(initial, last)])


def order_matrix(rows, transposed):
    length = rows // CHUNKS
    first = lax.broadcasted_iota(jnp.int32, (rows, rows), 0)
    second = lax.broadcasted_iota(jnp.int32, (rows, rows), 1)
    mixed, position = (second, first) if transposed else (first, second)
    hit = position == (mixed % CHUNKS) * length + mixed // CHUNKS
    return hit.astype(jnp.float32).astype(jnp.bfloat16)


def turn(angle):
    count = (angle * 0.6366197723675814 + 0.5).astype(jnp.int32)
    whole = count.astype(jnp.float32)
    rest = angle - whole * 1.5703125
    rest = rest - whole * 4.837512969970703125e-4
    rest = rest - whole * 7.54978995489188216e-8
    square = rest * rest
    sine = rest + rest * square * (
        -1.6666654611e-1 + square * (8.3321608736e-3 + square * -1.9515295891e-4)
    )
    less = square * (
        -0.5
        + square
        * (4.166664568298827e-2 + square * (-1.388731625493765e-3 + square * 2.443315711809948e-5))
    )
    cosine = 1.0 + less
    odd = (count & 1) == 1
    sin_out = jnp.where(odd, cosine, sine)
    cos_out = jnp.where(odd, sine, cosine)
    sin_out = jnp.where((count & 2) == 2, -sin_out, sin_out)
    cos_out = jnp.where(((count + 1) & 2) == 2, -cos_out, cos_out)
    less_out = jnp.where((count & 3) == 0, less, cos_out - 1.0)
    return less_out, cos_out, sin_out


def scan_kernel(
    x_ref, step_ref, spread_ref, lam_ref, high_ref, low_ref,
    are_ref, aim_ref, sre_ref, sim_ref, chunk_ref, total_ref,
    wide_ref, drive_ref,
):
    rows = x_ref.shape[0]
    width = lam_ref.shape[2]
    order = order_matrix(rows, False)
    x = jnp.dot(order, x_ref[...], preferred_element_type=jnp.float32).astype(jnp.bfloat16)
    drive_ref[...] = jnp.dot(x, high_ref[0], preferred_element_type=jnp.float32) + jnp.dot(
        x, low_ref[0], preferred_element_type=jnp.float32
    )
    wide_ref[...] = jnp.dot(
        step_ref[0], spread_ref[...], precision=lax.Precision.HIGHEST,
        preferred_element_type=jnp.float32,
    )

    def one(i, carry):
        here = pl.ds(pl.multiple_of(i * CHUNKS, CHUNKS), CHUNKS)
        results = []
        for j in range(width // LANES):
            a_re, a_im, s_re, s_im = carry[j]
            cols = slice(j * LANES, (j + 1) * LANES)
            step = wide_ref[here, cols]
            rate = lam_ref[0, 0:1, cols]
            freq = lam_ref[0, 1:2, cols]
            inv_re = lam_ref[0, 2:3, cols]
            inv_im = lam_ref[0, 3:4, cols]
            decay = -step * rate
            series = decay * (
                1.0 + decay * (0.5 + decay * (
                    1.0 / 6 + decay * (1.0 / 24 + decay * (1.0 / 120 + decay * (1.0 / 720)))
                ))
            )
            fall = jnp.where(decay > -0.25, series, jnp.exp(decay) - 1.0)
            modulus = 1.0 + fall
            modulus = jnp.where(decay > -0.25, modulus, jnp.exp(decay))
            cos_less, cosine, sine = turn(step * freq)
            t_re = modulus * cosine
            t_im = modulus * sine
            less = fall * cosine + cos_less
            f_re = less * inv_re - t_im * inv_im
            f_im = less * inv_im + t_im * inv_re
            d_re = drive_ref[here, cols]
            d_im = drive_ref[here, slice(width + j * LANES, width + (j + 1) * LANES)]
            p_re = f_re * d_re - f_im * d_im
            p_im = f_re * d_im + f_im * d_re
            s_re, s_im = t_re * s_re - t_im * s_im + p_re, t_re * s_im + t_im * s_re + p_im
            a_re, a_im = t_re * a_re - t_im * a_im, t_re * a_im + t_im * a_re
            are_ref[0, here, cols] = a_re
            aim_ref[0, here, cols] = a_im
            sre_ref[0, here, cols] = s_re
            sim_ref[0, here, cols] = s_im
            results.append((a_re, a_im, s_re, s_im))
        return tuple(results)

    ones = jnp.ones((CHUNKS, LANES), jnp.float32)
    zeros = jnp.zeros((CHUNKS, LANES), jnp.float32)
    start = tuple((ones, zeros, zeros, zeros) for _ in range(width // LANES))
    ends = lax.fori_loop(0, rows // CHUNKS, one, start)
    place = lax.broadcasted_iota(jnp.int32, (CHUNKS, LANES), 0)
    for j in range(width // LANES):
        cols = slice(j * LANES, (j + 1) * LANES)
        current = (ones[0:1], zeros[0:1], zeros[0:1], zeros[0:1])
        kept = [zeros] * 4
        for c in range(CHUNKS):
            kept = [jnp.where(place == c, v, k) for v, k in zip(current, kept)]
            t_re, t_im, p_re, p_im = (e[c : c + 1] for e in ends[j])
            a_re, a_im, s_re, s_im = current
            current = (
                t_re * a_re - t_im * a_im,
                t_re * a_im + t_im * a_re,
                t_re * s_re - t_im * s_im + p_re,
                t_re * s_im + t_im * s_re + p_im,
            )
        for q in range(4):
            chunk_ref[0, q, :, cols] = kept[q]
            total_ref[0, q : q + 1, cols] = current[q]


def read_kernel(
    are_ref, aim_ref, sre_ref, sim_ref, chunk_ref, enter_ref, x_ref, skip_ref, high_ref, low_ref,
    out_ref, state_ref,
):
    rows = x_ref.shape[0]
    width = are_ref.shape[2]
    e_re = enter_ref[0, 0:1, :]
    e_im = enter_ref[0, 1:2, :]
    a_re, a_im = chunk_ref[0, 0], chunk_ref[0, 1]
    c_re = a_re * e_re - a_im * e_im + chunk_ref[0, 2]
    c_im = a_re * e_im + a_im * e_re + chunk_ref[0, 3]

    def one(i, carry):
        here = pl.ds(pl.multiple_of(i * CHUNKS, CHUNKS), CHUNKS)
        a_re = are_ref[0, here, :]
        a_im = aim_ref[0, here, :]
        state_ref[here, 0:width] = sre_ref[0, here, :] + a_re * c_re - a_im * c_im
        state_ref[here, width : 2 * width] = sim_ref[0, here, :] + a_re * c_im + a_im * c_re
        return carry

    lax.fori_loop(0, rows // CHUNKS, one, 0)
    state = state_ref[...]
    high = state.astype(jnp.bfloat16)
    low = (state - high.astype(jnp.float32)).astype(jnp.bfloat16)
    read = (
        jnp.dot(high, high_ref[0], preferred_element_type=jnp.float32)
        + jnp.dot(low, high_ref[0], preferred_element_type=jnp.float32)
        + jnp.dot(high, low_ref[0], preferred_element_type=jnp.float32)
    )
    x = jnp.dot(order_matrix(rows, False), x_ref[...], preferred_element_type=jnp.float32)
    out = jax.nn.gelu(read + skip_ref[...] * x).astype(jnp.bfloat16)
    out_ref[...] = jnp.dot(
        order_matrix(rows, True), out, preferred_element_type=jnp.float32
    ).astype(jnp.bfloat16)


def conv_kernel_body(gated_ref, before_ref, taps_ref, gain_ref, out_ref, pad_ref):
    rows = gated_ref.shape[0]
    lead = before_ref.shape[0]
    count = taps_ref.shape[0]
    pad_ref[0:lead, :] = before_ref[...].astype(jnp.float32)
    pad_ref[lead:, :] = gated_ref[...].astype(jnp.float32)
    slab = 64
    for r in range(0, rows, slab):
        total = jnp.zeros((slab, LANES), jnp.float32)
        for k in range(count):
            begin = r + lead - (count - 1) + k
            total = total + taps_ref[k : k + 1, :] * pad_ref[begin : begin + slab, :]
        center = total - jnp.mean(total, axis=1, keepdims=True)
        spread = jnp.mean(center * center, axis=1, keepdims=True)
        value = center * lax.rsqrt(spread + 1e-05) * gain_ref[...]
        out_ref[r : r + slab, :] = (value * jax.nn.sigmoid(value)).astype(jnp.bfloat16)


def split(value):
    high = value.astype(jnp.bfloat16)
    low = (value - high.astype(jnp.float32)).astype(jnp.bfloat16)
    return high, low


def cost(flops, size):
    return pl.CostEstimate(flops=flops, bytes_accessed=size, transcendentals=0)


def ring_order(p, n):
    if n != 4:
        return p
    return p + lax.div(p, 2) * (1 - 2 * lax.rem(p, 2))


def gather_kernel(sizes, own_ref, out_ref, send_sem, recv_sem, local_sem):
    rows = own_ref.shape[0]
    s = lax.axis_index("sp")
    f = lax.axis_index("fs")
    spots = {"sp": s, "fs": ring_order(f, sizes["fs"])}

    def index(axis, position):
        return position if axis == "sp" else ring_order(position, sizes["fs"])

    def neighbours(axis):
        n, me = sizes[axis], spots[axis]
        return lax.rem(me + 1, n), lax.rem(me + n - 1, n)

    barrier = pltpu.get_barrier_semaphore()
    for axis in ("sp", "fs"):
        for position in neighbours(axis):
            pl.semaphore_signal(
                barrier, inc=1, device_id={axis: index(axis, position)},
                device_id_type=pl.DeviceIdType.MESH,
            )
    pl.semaphore_wait(barrier, 4)

    local = pltpu.make_async_copy(own_ref, out_ref.at[s, f], local_sem)
    local.start()
    started = []

    def hop(axis, phase, half, h):
        n, me = sizes[axis], spots[axis]
        base, size = half * (rows // 2), rows // 2
        if 2 * h == n:
            spans = ((base, size // 2), (base + size // 2, size // 2))
        else:
            spans = ((base, size), (base, size))
        blocks = (lax.rem(me + n - (h - 1), n), lax.rem(me + h - 1, n))
        copies = []
        for position, block, span in zip(neighbours(axis), blocks, spans):
            where = pl.ds(*span)
            at = index(axis, block)
            if phase == 0:
                view = out_ref.at[at, f, where] if axis == "sp" else out_ref.at[s, at, where]
            else:
                view = out_ref.at[at, :, where] if axis == "sp" else out_ref.at[:, at, where]
            slot = len(started)
            copy = pltpu.make_async_remote_copy(
                src_ref=own_ref.at[where] if phase == 0 and h == 1 else view,
                dst_ref=view,
                send_sem=send_sem.at[slot],
                recv_sem=recv_sem.at[slot],
                device_id={axis: index(axis, position)},
                device_id_type=pl.DeviceIdType.MESH,
            )
            copy.start()
            started.append(copy)
            copies.append(copy)
        return copies

    for phase in range(2):
        routes = (("sp", "fs")[phase], 0), (("fs", "sp")[phase], 1)
        if phase == 1:
            local.wait()
        for h in range(1, max(sizes.values()) // 2 + 1):
            flying = []
            for axis, half in routes:
                if h <= sizes[axis] // 2:
                    flying += hop(axis, phase, half, h)
            for copy in flying:
                copy.wait_recv()
    for copy in started:
        copy.wait_send()


def gathered_rows(own):
    sizes = {axis: lax.axis_size(axis) for axis in ("sp", "fs")}
    copies = 4 * sum(n // 2 for n in sizes.values())
    out = pl.pallas_call(
        functools.partial(gather_kernel, sizes),
        in_specs=[pl.BlockSpec(memory_space=pl.ANY)],
        out_specs=pl.BlockSpec(memory_space=pl.ANY),
        out_shape=jax.ShapeDtypeStruct((sizes["sp"], sizes["fs"]) + own.shape, own.dtype),
        scratch_shapes=[
            pltpu.SemaphoreType.DMA((copies,)),
            pltpu.SemaphoreType.DMA((copies,)),
            pltpu.SemaphoreType.DMA,
        ],
        compiler_params=pltpu.CompilerParams(collective_id=0, has_side_effects=True),
        cost_estimate=cost(10**6, 100 * own.size),
        name="gather",
    )(own)
    return out.reshape(-1, own.shape[1])


def body(
    stream, norm_gain, value_proj, gate_proj, state_proj, conv_kernel, conv_gain, decay_rate,
    frequency, log_step, step_gain, drive_matrix, read_matrix, skip_gain, start_state,
    merge_conv, merge_state,
):
    rows = stream.shape[1]
    groups, states = decay_rate.shape
    per = drive_matrix.shape[3]
    pack = min(groups, LANES // per)
    blocks = groups // pack
    width = pack * states
    chans = pack * per
    f32 = jnp.float32

    proj_whole = gathered_rows(jnp.concatenate([state_proj, value_proj, gate_proj], axis=1))
    conv_merge = lax.all_gather(merge_conv, ("sp", "fs"), axis=0, tiled=True)
    state_merge = lax.all_gather(merge_state, ("sp", "fs"), axis=0, tiled=True)

    widened = stream[0].astype(f32)
    inverse = lax.rsqrt(jnp.mean(widened * widened, axis=1, keepdims=True) + 1e-06)
    normed = (widened * inverse * norm_gain).astype(jnp.bfloat16)

    step = (jnp.exp(log_step)[:, None] * step_gain[0]).reshape(
        blocks, pack, CHUNKS, rows // CHUNKS
    )
    step = jnp.transpose(step, (0, 3, 2, 1)).reshape(blocks, rows, pack)
    spread = jnp.repeat(jnp.eye(pack, dtype=f32), states, axis=1)
    magnitude = decay_rate * decay_rate + frequency * frequency
    lam = jnp.stack(
        [decay_rate, frequency, -decay_rate / magnitude, -frequency / magnitude]
    ).reshape(4, blocks, width)
    lam = jnp.transpose(lam, (1, 0, 2))
    same = jnp.eye(pack, dtype=f32)
    drive = jnp.transpose(drive_matrix.reshape(2, blocks, pack, states, per), (1, 2, 4, 0, 3))
    drive = drive[:, :, :, :, None, :] * same[None, :, None, None, :, None]
    drive_high, drive_low = split(drive.reshape(blocks, chans, 2 * width))
    signed = jnp.stack([read_matrix[0], -read_matrix[1]])
    read = jnp.transpose(signed.reshape(2, blocks, pack, per, states), (1, 0, 2, 4, 3))
    read = read[:, :, :, :, None, :] * same[None, None, :, None, :, None]
    read_high, read_low = split(read.reshape(blocks, 2 * width, chans))

    pre = jnp.dot(normed, proj_whole, preferred_element_type=f32)
    scan_width, conv_width = state_proj.shape[1], value_proj.shape[1]
    scan_input = pre[:, :scan_width].astype(jnp.bfloat16)

    def slab(*shape):
        return pl.BlockSpec((1,) + shape, lambda b: (b,) + (0,) * len(shape))

    chan_spec = pl.BlockSpec((rows, chans), lambda b: (0, b))
    row_spec = pl.BlockSpec((1, chans), lambda b: (0, b))
    wide = jax.ShapeDtypeStruct((blocks, rows, width), f32)
    *running, chunk, total = pl.pallas_call(
        scan_kernel,
        grid=(blocks,),
        in_specs=[
            chan_spec, slab(rows, pack), pl.BlockSpec((pack, width), lambda b: (0, 0)),
            slab(4, width), slab(chans, 2 * width), slab(chans, 2 * width),
        ],
        out_specs=[slab(rows, width)] * 4 + [slab(4, CHUNKS, width), slab(4, width)],
        out_shape=[wide] * 4 + [
            jax.ShapeDtypeStruct((blocks, 4, CHUNKS, width), f32),
            jax.ShapeDtypeStruct((blocks, 4, width), f32),
        ],
        scratch_shapes=[pltpu.VMEM((rows, width), f32), pltpu.VMEM((rows, 2 * width), f32)],
        cost_estimate=cost(60 * rows * blocks * width * 30, 16 * rows * blocks * width),
        name="scan",
    )(scan_input, step, spread, lam, drive_high, drive_low)

    place = lax.axis_index("sp")
    arrived = [
        (hop, shifted(total, "sp", hop)) for hop in range(lax.axis_size("sp") - 1, 0, -1)
    ]
    begin = start_state[:, 0].reshape(2, blocks, width)
    enter_re, enter_im = begin[0], begin[1]
    for hop, part in arrived:
        t_re, t_im, p_re, p_im = (part[:, q] for q in range(4))
        known = place >= hop
        next_re = t_re * enter_re - t_im * enter_im + p_re
        next_im = t_re * enter_im + t_im * enter_re + p_im
        enter_re = jnp.where(known, next_re, enter_re)
        enter_im = jnp.where(known, next_im, enter_im)
    enter = jnp.stack([enter_re, enter_im], axis=1)

    state_out = pl.pallas_call(
        read_kernel,
        grid=(blocks,),
        in_specs=[slab(rows, width)] * 4 + [
            slab(4, CHUNKS, width), slab(2, width), chan_spec, row_spec,
            slab(2 * width, chans), slab(2 * width, chans),
        ],
        out_specs=chan_spec,
        out_shape=jax.ShapeDtypeStruct((rows, groups * per), jnp.bfloat16),
        scratch_shapes=[pltpu.VMEM((rows, 2 * width), f32)],
        cost_estimate=cost(60 * rows * blocks * width * 10, 16 * rows * blocks * width),
        name="read",
    )(*running, chunk, enter, scan_input, skip_gain[None], read_high, read_low)

    value_pre = pre[:, scan_width : scan_width + conv_width]
    gate_pre = pre[:, scan_width + conv_width :]
    gated = (value_pre * jax.nn.sigmoid(gate_pre)).astype(jnp.bfloat16)
    lead = -(-(conv_kernel.shape[0] - 1) // 16) * 16
    before = shifted(gated[rows - lead :], "sp", 1)
    head_spec = lambda n: pl.BlockSpec((n, HEAD_CH), lambda h: (0, h))
    conv_out = pl.pallas_call(
        conv_kernel_body,
        grid=(conv_width // HEAD_CH,),
        in_specs=[
            head_spec(rows), head_spec(lead), head_spec(conv_kernel.shape[0]), head_spec(1),
        ],
        out_specs=head_spec(rows),
        out_shape=jax.ShapeDtypeStruct((rows, conv_width), jnp.bfloat16),
        scratch_shapes=[pltpu.VMEM((rows + lead, HEAD_CH), f32)],
        cost_estimate=cost(rows * conv_width * 2000, 4 * rows * conv_width),
        name="conv",
    )(gated, before, conv_kernel.astype(f32), conv_gain[None])

    contract = (((1,), (1,)), ((), ()))
    conv_term = lax.dot_general(conv_out, conv_merge, contract, preferred_element_type=f32)
    state_term = lax.dot_general(state_out, state_merge, contract, preferred_element_type=f32)
    mixed = lax.psum_scatter(
        (conv_term + state_term).astype(jnp.bfloat16), "tp", scatter_dimension=0, tiled=True
    )
    return mixed[None]


def solution(mesh):
    return jax.shard_map(
        body,
        mesh=mesh,
        in_specs=(
            P("fs", "sp", None),
            P(),
            P(("sp", "fs"), "tp"),
            P(("sp", "fs"), "tp"),
            P(("sp", "fs"), "tp"),
            P(None, "tp"),
            P("tp"),
            P("tp", None),
            P("tp", None),
            P("tp"),
            P("fs", "tp", "sp"),
            P(None, "tp", None, None),
            P(None, "tp", None, None),
            P("tp"),
            P(None, "fs", "tp", None),
            P(("sp", "fs"), "tp"),
            P(("sp", "fs"), "tp"),
        ),
        out_specs=P("fs", ("sp", "tp"), None),
        check_vma=False,
    )
```

```python
import functools

import jax
import jax.numpy as jnp
from jax import lax
from jax.experimental import pallas as pl
from jax.experimental.pallas import tpu as pltpu
from jax.sharding import PartitionSpec as P

HEAD_CH = 128
LANES = 128
CHUNKS = 8


def shifted(value, axis, steps):
    count = lax.axis_size(axis)
    initial, last = (max(0, -steps), min(count, count - steps))
    return lax.ppermute(value, axis, [(source, source + steps) for source in range(initial, last)])


def order_matrix(rows, transposed):
    length = rows // CHUNKS
    first = lax.broadcasted_iota(jnp.int32, (rows, rows), 0)
    second = lax.broadcasted_iota(jnp.int32, (rows, rows), 1)
    mixed, position = (second, first) if transposed else (first, second)
    hit = position == (mixed % CHUNKS) * length + mixed // CHUNKS
    return hit.astype(jnp.float32).astype(jnp.bfloat16)


def turn(angle):
    count = (angle * 0.6366197723675814 + 0.5).astype(jnp.int32)
    whole = count.astype(jnp.float32)
    rest = angle - whole * 1.5703125
    rest = rest - whole * 4.837512969970703125e-4
    rest = rest - whole * 7.54978995489188216e-8
    square = rest * rest
    sine = rest + rest * square * (
        -1.6666654611e-1 + square * (8.3321608736e-3 + square * -1.9515295891e-4)
    )
    less = square * (
        -0.5
        + square
        * (4.166664568298827e-2 + square * (-1.388731625493765e-3 + square * 2.443315711809948e-5))
    )
    cosine = 1.0 + less
    odd = (count & 1) == 1
    sin_out = jnp.where(odd, cosine, sine)
    cos_out = jnp.where(odd, sine, cosine)
    sin_out = jnp.where((count & 2) == 2, -sin_out, sin_out)
    cos_out = jnp.where(((count + 1) & 2) == 2, -cos_out, cos_out)
    less_out = jnp.where((count & 3) == 0, less, cos_out - 1.0)
    return less_out, cos_out, sin_out


def spread_groups(compact, pack, per):
    chans, states = compact.shape
    wide = jnp.concatenate([compact] * pack, axis=1)
    row = lax.broadcasted_iota(jnp.int32, wide.shape, 0) // per
    column = lax.broadcasted_iota(jnp.int32, wide.shape, 1) // states
    return jnp.where(row == column, wide, 0.0)


def scan_kernel(
    x_ref, step_ref, spread_ref, lam_ref, matrix_ref,
    are_ref, aim_ref, sre_ref, sim_ref, chunk_ref, total_ref,
    wide_ref, drive_ref,
):
    rows = x_ref.shape[0]
    width = lam_ref.shape[2]
    order = order_matrix(rows, False)
    x = jnp.dot(order, x_ref[...], preferred_element_type=jnp.float32).astype(jnp.bfloat16)
    pack = step_ref.shape[2]
    for q in range(2):
        high, low = split(spread_groups(matrix_ref[q, 0], pack, x_ref.shape[1] // pack))
        drive_ref[:, q * width : (q + 1) * width] = jnp.dot(
            x, high, preferred_element_type=jnp.float32
        ) + jnp.dot(x, low, preferred_element_type=jnp.float32)
    wide_ref[...] = jnp.dot(
        step_ref[0], spread_ref[...], precision=lax.Precision.HIGHEST,
        preferred_element_type=jnp.float32,
    )

    def one(i, carry):
        here = pl.ds(pl.multiple_of(i * CHUNKS, CHUNKS), CHUNKS)
        results = []
        for j in range(width // LANES):
            a_re, a_im, s_re, s_im = carry[j]
            cols = slice(j * LANES, (j + 1) * LANES)
            step = wide_ref[here, cols]
            rate = lam_ref[0, 0:1, cols]
            freq = lam_ref[0, 1:2, cols]
            inv_re = lam_ref[0, 2:3, cols]
            inv_im = lam_ref[0, 3:4, cols]
            decay = -step * rate
            series = decay * (
                1.0 + decay * (0.5 + decay * (
                    1.0 / 6 + decay * (1.0 / 24 + decay * (1.0 / 120 + decay * (1.0 / 720)))
                ))
            )
            fall = jnp.where(decay > -0.25, series, jnp.exp(decay) - 1.0)
            modulus = 1.0 + fall
            modulus = jnp.where(decay > -0.25, modulus, jnp.exp(decay))
            cos_less, cosine, sine = turn(step * freq)
            t_re = modulus * cosine
            t_im = modulus * sine
            less = fall * cosine + cos_less
            f_re = less * inv_re - t_im * inv_im
            f_im = less * inv_im + t_im * inv_re
            d_re = drive_ref[here, cols]
            d_im = drive_ref[here, slice(width + j * LANES, width + (j + 1) * LANES)]
            p_re = f_re * d_re - f_im * d_im
            p_im = f_re * d_im + f_im * d_re
            s_re, s_im = t_re * s_re - t_im * s_im + p_re, t_re * s_im + t_im * s_re + p_im
            a_re, a_im = t_re * a_re - t_im * a_im, t_re * a_im + t_im * a_re
            are_ref[0, here, cols] = a_re
            aim_ref[0, here, cols] = a_im
            sre_ref[0, here, cols] = s_re
            sim_ref[0, here, cols] = s_im
            results.append((a_re, a_im, s_re, s_im))
        return tuple(results)

    ones = jnp.ones((CHUNKS, LANES), jnp.float32)
    zeros = jnp.zeros((CHUNKS, LANES), jnp.float32)
    start = tuple((ones, zeros, zeros, zeros) for _ in range(width // LANES))
    ends = lax.fori_loop(0, rows // CHUNKS, one, start)
    place = lax.broadcasted_iota(jnp.int32, (CHUNKS, LANES), 0)
    for j in range(width // LANES):
        cols = slice(j * LANES, (j + 1) * LANES)
        current = (ones[0:1], zeros[0:1], zeros[0:1], zeros[0:1])
        kept = [zeros] * 4
        for c in range(CHUNKS):
            kept = [jnp.where(place == c, v, k) for v, k in zip(current, kept)]
            t_re, t_im, p_re, p_im = (e[c : c + 1] for e in ends[j])
            a_re, a_im, s_re, s_im = current
            current = (
                t_re * a_re - t_im * a_im,
                t_re * a_im + t_im * a_re,
                t_re * s_re - t_im * s_im + p_re,
                t_re * s_im + t_im * s_re + p_im,
            )
        for q in range(4):
            chunk_ref[0, q, :, cols] = kept[q]
            total_ref[0, q : q + 1, cols] = current[q]


def read_kernel(
    are_ref, aim_ref, sre_ref, sim_ref, chunk_ref, enter_ref, x_ref, skip_ref, matrix_ref,
    out_ref, state_ref,
):
    rows = x_ref.shape[0]
    width = are_ref.shape[2]
    e_re = enter_ref[0, 0:1, :]
    e_im = enter_ref[0, 1:2, :]
    a_re, a_im = chunk_ref[0, 0], chunk_ref[0, 1]
    c_re = a_re * e_re - a_im * e_im + chunk_ref[0, 2]
    c_im = a_re * e_im + a_im * e_re + chunk_ref[0, 3]

    def one(i, carry):
        here = pl.ds(pl.multiple_of(i * CHUNKS, CHUNKS), CHUNKS)
        a_re = are_ref[0, here, :]
        a_im = aim_ref[0, here, :]
        state_ref[here, 0:width] = sre_ref[0, here, :] + a_re * c_re - a_im * c_im
        state_ref[here, width : 2 * width] = sim_ref[0, here, :] + a_re * c_im + a_im * c_re
        return carry

    lax.fori_loop(0, rows // CHUNKS, one, 0)
    pack = width // matrix_ref.shape[3]
    reads = []
    for q in range(2):
        high, low = split(state_ref[:, q * width : (q + 1) * width])
        major, minor = split(spread_groups(matrix_ref[q, 0], pack, x_ref.shape[1] // pack))
        reads.append(
            across(high, major) + across(low, major) + across(high, minor)
        )
    read = reads[0] - reads[1]
    x = jnp.dot(order_matrix(rows, False), x_ref[...], preferred_element_type=jnp.float32)
    out = jax.nn.gelu(read + skip_ref[...] * x).astype(jnp.bfloat16)
    out_ref[...] = jnp.dot(
        order_matrix(rows, True), out, preferred_element_type=jnp.float32
    ).astype(jnp.bfloat16)


def conv_kernel_body(gated_ref, before_ref, taps_ref, gain_ref, out_ref, pad_ref):
    rows = gated_ref.shape[0]
    lead = before_ref.shape[0]
    count = taps_ref.shape[0]
    pad_ref[0:lead, :] = before_ref[...].astype(jnp.float32)
    pad_ref[lead:, :] = gated_ref[...].astype(jnp.float32)
    slab = 64
    for r in range(0, rows, slab):
        total = jnp.zeros((slab, LANES), jnp.float32)
        for k in range(count):
            begin = r + lead - (count - 1) + k
            total = total + taps_ref[k : k + 1, :] * pad_ref[begin : begin + slab, :]
        center = total - jnp.mean(total, axis=1, keepdims=True)
        spread = jnp.mean(center * center, axis=1, keepdims=True)
        value = center * lax.rsqrt(spread + 1e-05) * gain_ref[...]
        out_ref[r : r + slab, :] = (value * jax.nn.sigmoid(value)).astype(jnp.bfloat16)


def across(left, right):
    return lax.dot_general(
        left, right, (((1,), (1,)), ((), ())), preferred_element_type=jnp.float32
    )


def split(value):
    high = value.astype(jnp.bfloat16)
    low = (value - high.astype(jnp.float32)).astype(jnp.bfloat16)
    return high, low


def cost(flops, size):
    return pl.CostEstimate(flops=flops, bytes_accessed=size, transcendentals=0)


def ring_order(p, n):
    if n != 4:
        return p
    return p + lax.div(p, 2) * (1 - 2 * lax.rem(p, 2))


def gather_kernel(sizes, own_ref, out_ref, send_sem, recv_sem, local_sem):
    rows = own_ref.shape[0]
    s = lax.axis_index("sp")
    f = lax.axis_index("fs")
    spots = {"sp": s, "fs": ring_order(f, sizes["fs"])}

    def index(axis, position):
        return position if axis == "sp" else ring_order(position, sizes["fs"])

    def neighbours(axis):
        n, me = sizes[axis], spots[axis]
        return lax.rem(me + 1, n), lax.rem(me + n - 1, n)

    barrier = pltpu.get_barrier_semaphore()
    for axis in ("sp", "fs"):
        for position in neighbours(axis):
            pl.semaphore_signal(
                barrier, inc=1, device_id={axis: index(axis, position)},
                device_id_type=pl.DeviceIdType.MESH,
            )
    pl.semaphore_wait(barrier, 4)

    local = pltpu.make_async_copy(own_ref, out_ref.at[s, f], local_sem)
    local.start()
    started = []

    def hop(axis, phase, half, h):
        n, me = sizes[axis], spots[axis]
        cut = rows * 5 // 8 // 32 * 32
        base, size = ((0, cut), (cut, rows - cut))[half]
        if 2 * h == n:
            spans = ((base, size // 2), (base + size // 2, size // 2))
        else:
            spans = ((base, size), (base, size))
        blocks = (lax.rem(me + n - (h - 1), n), lax.rem(me + h - 1, n))
        copies = []
        for position, block, span in zip(neighbours(axis), blocks, spans):
            where = pl.ds(*span)
            at = index(axis, block)
            if phase == 0:
                view = out_ref.at[at, f, where] if axis == "sp" else out_ref.at[s, at, where]
            else:
                view = out_ref.at[at, :, where] if axis == "sp" else out_ref.at[:, at, where]
            slot = len(started)
            copy = pltpu.make_async_remote_copy(
                src_ref=own_ref.at[where] if phase == 0 and h == 1 else view,
                dst_ref=view,
                send_sem=send_sem.at[slot],
                recv_sem=recv_sem.at[slot],
                device_id={axis: index(axis, position)},
                device_id_type=pl.DeviceIdType.MESH,
            )
            copy.start()
            started.append(copy)
            copies.append(copy)
        return copies

    for phase in range(2):
        routes = (("sp", "fs")[phase], 0), (("fs", "sp")[phase], 1)
        if phase == 1:
            local.wait()
        for h in range(1, max(sizes.values()) // 2 + 1):
            flying = []
            for axis, half in routes:
                if h <= sizes[axis] // 2:
                    flying += hop(axis, phase, half, h)
            for copy in flying:
                copy.wait_recv()
    for copy in started:
        copy.wait_send()


def gathered_rows(own):
    sizes = {axis: lax.axis_size(axis) for axis in ("sp", "fs")}
    copies = 4 * sum(n // 2 for n in sizes.values())
    out = pl.pallas_call(
        functools.partial(gather_kernel, sizes),
        in_specs=[pl.BlockSpec(memory_space=pl.ANY)],
        out_specs=pl.BlockSpec(memory_space=pl.ANY),
        out_shape=jax.ShapeDtypeStruct((sizes["sp"], sizes["fs"]) + own.shape, own.dtype),
        scratch_shapes=[
            pltpu.SemaphoreType.DMA((copies,)),
            pltpu.SemaphoreType.DMA((copies,)),
            pltpu.SemaphoreType.DMA,
        ],
        compiler_params=pltpu.CompilerParams(collective_id=0, has_side_effects=True),
        cost_estimate=cost(10**6, 100 * own.size),
        name="gather",
    )(own)
    return out.reshape(-1, own.shape[1])


def body(
    stream, norm_gain, value_proj, gate_proj, state_proj, conv_kernel, conv_gain, decay_rate,
    frequency, log_step, step_gain, drive_matrix, read_matrix, skip_gain, start_state,
    merge_conv, merge_state,
):
    rows = stream.shape[1]
    groups, states = decay_rate.shape
    per = drive_matrix.shape[3]
    pack = min(groups, LANES // per)
    blocks = groups // pack
    width = pack * states
    chans = pack * per
    f32 = jnp.float32

    proj_whole = gathered_rows(jnp.concatenate([state_proj, value_proj, gate_proj], axis=1))
    conv_merge = lax.all_gather(merge_conv, ("sp", "fs"), axis=0, tiled=True)
    state_merge = lax.all_gather(merge_state, ("sp", "fs"), axis=0, tiled=True)

    widened = stream[0].astype(f32)
    inverse = lax.rsqrt(jnp.mean(widened * widened, axis=1, keepdims=True) + 1e-06)
    normed = (widened * inverse * norm_gain).astype(jnp.bfloat16)

    step = (jnp.exp(log_step)[:, None] * step_gain[0]).reshape(
        blocks, pack, CHUNKS, rows // CHUNKS
    )
    step = jnp.transpose(step, (0, 3, 2, 1)).reshape(blocks, rows, pack)
    spread = jnp.repeat(jnp.eye(pack, dtype=f32), states, axis=1)
    magnitude = decay_rate * decay_rate + frequency * frequency
    lam = jnp.stack(
        [decay_rate, frequency, -decay_rate / magnitude, -frequency / magnitude]
    ).reshape(4, blocks, width)
    lam = jnp.transpose(lam, (1, 0, 2))
    drive = jnp.swapaxes(drive_matrix, 2, 3).reshape(2, blocks, chans, states)
    read = read_matrix.reshape(2, blocks, chans, states)

    pre = jnp.dot(normed, proj_whole, preferred_element_type=f32)
    scan_width, conv_width = state_proj.shape[1], value_proj.shape[1]
    scan_input = pre[:, :scan_width].astype(jnp.bfloat16)

    def slab(*shape):
        return pl.BlockSpec((1,) + shape, lambda b: (b,) + (0,) * len(shape))

    pair_spec = pl.BlockSpec((2, 1, chans, states), lambda b: (0, b, 0, 0))
    chan_spec = pl.BlockSpec((rows, chans), lambda b: (0, b))
    row_spec = pl.BlockSpec((1, chans), lambda b: (0, b))
    wide = jax.ShapeDtypeStruct((blocks, rows, width), f32)
    *running, chunk, total = pl.pallas_call(
        scan_kernel,
        grid=(blocks,),
        in_specs=[
            chan_spec, slab(rows, pack), pl.BlockSpec((pack, width), lambda b: (0, 0)),
            slab(4, width), pair_spec,
        ],
        out_specs=[slab(rows, width)] * 4 + [slab(4, CHUNKS, width), slab(4, width)],
        out_shape=[wide] * 4 + [
            jax.ShapeDtypeStruct((blocks, 4, CHUNKS, width), f32),
            jax.ShapeDtypeStruct((blocks, 4, width), f32),
        ],
        scratch_shapes=[pltpu.VMEM((rows, width), f32), pltpu.VMEM((rows, 2 * width), f32)],
        cost_estimate=cost(60 * rows * blocks * width * 30, 16 * rows * blocks * width),
        name="scan",
    )(scan_input, step, spread, lam, drive)

    place = lax.axis_index("sp")
    arrived = [
        (hop, shifted(total, "sp", hop)) for hop in range(lax.axis_size("sp") - 1, 0, -1)
    ]
    begin = start_state[:, 0].reshape(2, blocks, width)
    enter_re, enter_im = begin[0], begin[1]
    for hop, part in arrived:
        t_re, t_im, p_re, p_im = (part[:, q] for q in range(4))
        known = place >= hop
        next_re = t_re * enter_re - t_im * enter_im + p_re
        next_im = t_re * enter_im + t_im * enter_re + p_im
        enter_re = jnp.where(known, next_re, enter_re)
        enter_im = jnp.where(known, next_im, enter_im)
    enter = jnp.stack([enter_re, enter_im], axis=1)

    state_out = pl.pallas_call(
        read_kernel,
        grid=(blocks,),
        in_specs=[slab(rows, width)] * 4 + [
            slab(4, CHUNKS, width), slab(2, width), chan_spec, row_spec,
            pair_spec,
        ],
        out_specs=chan_spec,
        out_shape=jax.ShapeDtypeStruct((rows, groups * per), jnp.bfloat16),
        scratch_shapes=[pltpu.VMEM((rows, 2 * width), f32)],
        cost_estimate=cost(60 * rows * blocks * width * 10, 16 * rows * blocks * width),
        name="read",
    )(*running, chunk, enter, scan_input, skip_gain[None], read)

    value_pre = pre[:, scan_width : scan_width + conv_width]
    gate_pre = pre[:, scan_width + conv_width :]
    gated = (value_pre * jax.nn.sigmoid(gate_pre)).astype(jnp.bfloat16)
    lead = -(-(conv_kernel.shape[0] - 1) // 16) * 16
    before = shifted(gated[rows - lead :], "sp", 1)
    head_spec = lambda n: pl.BlockSpec((n, HEAD_CH), lambda h: (0, h))
    conv_out = pl.pallas_call(
        conv_kernel_body,
        grid=(conv_width // HEAD_CH,),
        in_specs=[
            head_spec(rows), head_spec(lead), head_spec(conv_kernel.shape[0]), head_spec(1),
        ],
        out_specs=head_spec(rows),
        out_shape=jax.ShapeDtypeStruct((rows, conv_width), jnp.bfloat16),
        scratch_shapes=[pltpu.VMEM((rows + lead, HEAD_CH), f32)],
        cost_estimate=cost(rows * conv_width * 2000, 4 * rows * conv_width),
        name="conv",
    )(gated, before, conv_kernel.astype(f32), conv_gain[None])

    contract = (((1,), (1,)), ((), ()))
    conv_term = lax.dot_general(conv_out, conv_merge, contract, preferred_element_type=f32)
    state_term = lax.dot_general(state_out, state_merge, contract, preferred_element_type=f32)
    mixed = lax.psum_scatter(
        (conv_term + state_term).astype(jnp.bfloat16), "tp", scatter_dimension=0, tiled=True
    )
    return mixed[None]


def solution(mesh):
    return jax.shard_map(
        body,
        mesh=mesh,
        in_specs=(
            P("fs", "sp", None),
            P(),
            P(("sp", "fs"), "tp"),
            P(("sp", "fs"), "tp"),
            P(("sp", "fs"), "tp"),
            P(None, "tp"),
            P("tp"),
            P("tp", None),
            P("tp", None),
            P("tp"),
            P("fs", "tp", "sp"),
            P(None, "tp", None, None),
            P(None, "tp", None, None),
            P("tp"),
            P(None, "fs", "tp", None),
            P(("sp", "fs"), "tp"),
            P(("sp", "fs"), "tp"),
        ),
        out_specs=P("fs", ("sp", "tp"), None),
        check_vma=False,
    )
```
